32 devices in a mesh: ep: 8 (over z, core), tp: 4 (over y, x).
Axes of the slice: x: 2, y: 2, z: 4, core: 2. Of those that a mesh axis runs over, the one named last changes fastest.
Arguments:
- q_latent: bfloat16 [1536, 512], P('ep'), may hold values from -6 to 6
- kv_latent: bfloat16 [1536, 256], P('ep'), may hold values from -6 to 6
- rope_key: bfloat16 [1536, 64], P('ep'), may hold values from -900 to 900
- q_gain: float32 [512], replicated, may hold values from 0.1 to 1.9
- kv_gain: float32 [256], replicated, may hold values from 0.1 to 1.9
- w_query: bfloat16 [512, 3072], P(None, 'tp'), may hold values from -0.25 to 0.25
- w_key: bfloat16 [256, 2048], P(None, 'tp'), may hold values from -0.375 to 0.375
- w_value: bfloat16 [256, 2048], P(None, 'tp'), may hold values from -0.375 to 0.375
- w_mix_out: bfloat16 [2048, 2048], P('tp'), may hold values from -0.125 to 0.125
- expert_in: bfloat16 [1024, 2048], P('ep'), may hold values from -6 to 6
- norm_gain: float32 [2048], replicated, may hold values from 0.1 to 1.9
- routes: int32 [1024, 2], P('ep'), may hold values from 0 to 7, all different within a row; in each aligned block of 128 rows (0 to 127, 128 to 255, ...) at most 64 rows name the same one
- route_scores: float32 [1024, 2], P('ep'), may hold values from 0.05 to 1
- w_gate: bfloat16 [8, 2048, 4096], P('ep', None, 'tp'), may hold values from -0.125 to 0.125
- w_up: bfloat16 [8, 2048, 4096], P('ep', None, 'tp'), may hold values from -0.125 to 0.125
- w_down: bfloat16 [8, 4096, 2048], P('ep', 'tp'), may hold values from -0.125 to 0.125
Outputs:
- mixed: bfloat16 [1536, 2048], P(('ep', 'tp'))
- expert_out: bfloat16 [1024, 2048], P('ep', 'tp')
The draws below stay inside these ranges and needn't reach their ends.
Inputs may be any that keep to these rules, and one draw needn't show every extreme that they name: `routes`: each row names 2 different experts; in the rows of one index of ep no expert is named by more than 64 rows, a bound that some block reaches.
All inputs are finite; a program needn't handle non-finite values.
Results may differ from the reference program's by a relative error of at most 0.03.
The reference program's roundings to bfloat16 on the way count: a program that leaves them out, or rounds other values in their place, can miss the bound.
Values may be sent and summed in bfloat16 or wider, within the bound.
A program may use at most 64 MiB of HBM per device.

```python
import math
import jax
import jax.numpy as jnp
import numpy as np
from jax import lax

D = 2048
HEADS = 16
QR = 512
KVR = 256
NOPE = 128
ROPE = 64
VDIM = 128
FF = 4096
TOP = 2
TOKA = 192
TOKB = 128
EXPERTS = 8
CAP = 64
N_EP = 8
N_TP = 4


def draw_rope_key(key, part):
    length = TOKA * N_EP
    base = jnp.clip(jax.random.normal(jax.random.fold_in(key, 11), (length, ROPE), jnp.float32), -6.0, 6.0)
    return base.astype(jnp.bfloat16)


def strengthened(array, rng, source, target, shards_of, factor):
    def block_of(axis_at):
        return (jnp.arange(array.shape[axis_at]) // (array.shape[axis_at] // shards_of)).reshape((-1,) + (1,) * (array.ndim - 1 - axis_at))

    first = jax.random.permutation(rng, shards_of)[block_of(target)]
    far = (block_of(target) + shards_of // 2) % shards_of
    return jnp.where((block_of(source) == first) | (block_of(source) == far), factor * array, array)


def level_of(key, extent, cuts, least, top_value):
    level, own = 1.0, jax.random.fold_in(key, 6)
    for axis_at, shards_of in cuts:
        heights = jnp.exp(jax.random.uniform(jax.random.fold_in(own, axis_at), (shards_of,), jnp.float32, least / len(cuts), top_value / len(cuts)))
        level = level * jnp.repeat(heights, extent[axis_at] // shards_of).reshape([-1 if axis == axis_at else 1 for axis in range(len(extent))])
    return level


def assign_block(key, own, number, rows, count, top, bound, skew):
    ranking = jax.random.permutation(key, count)
    heavy_load, usual = load_shares(count, rows * top, bound, skew, True), load_shares(count, rows * top, bound, skew, False)
    places = jnp.arange(count)

    def named(tallies, offset_by):
        used = int((tallies > 0).sum())
        fixed = max(1, used // 4)
        moved = fixed + (places - fixed + offset_by * (used - fixed)) % max(1, count - fixed)
        return jnp.zeros((count,), jnp.int32).at[ranking[jnp.where(places < fixed, places, moved)]].set(jnp.asarray(tallies, jnp.int32))

    tallies = jnp.where(number % 4 == 0, named(heavy_load, number // 4), named(usual, number - number // 4 - 1))
    mixed = jax.random.permutation(jax.random.fold_in(own, 3), count)
    source_of, taker = mixed[0:count // 2 * 2:2], mixed[1:count // 2 * 2:2]
    room = jnp.minimum(tallies[source_of] - 1, bound - tallies[taker]) // 2
    room = jnp.where((source_of == ranking[0]) | (taker == ranking[0]) | (tallies[taker] == 0), 0, jnp.maximum(room, 0))
    moved = jax.random.randint(jax.random.fold_in(own, 4), (count // 2,), 0, 1 << 20) % (room + 1)
    tallies = tallies.at[source_of].add(-moved).at[taker].add(moved)
    labels = jnp.searchsorted(jnp.cumsum(tallies), jnp.arange(rows * top), side="right").astype(jnp.int32)
    listing = labels.reshape(top, rows).T
    listing = listing[jax.random.permutation(jax.random.fold_in(own, 1), rows)]
    offset_by = jax.random.randint(jax.random.fold_in(own, 2), (rows, 1), 0, top)
    return jnp.take_along_axis(listing, (jnp.arange(top)[None, :] + offset_by) % top, axis=1)


def load_shares(amount, total, limit, lean, full):
    portions = [(1 << 20) // math.isqrt(grade ** lean) + 1 for grade in range(1, amount + 1)]
    largest = limit if full else min(limit, max(-(-total // amount), total * portions[0] // sum(portions)))
    least = 1 if total - largest >= amount - 1 else 0
    counts, surplus = [largest] + [least] * (amount - 1), total - largest - least * (amount - 1)
    while surplus > 0:
        movable = [i for i in range(1, amount) if counts[i] < largest] or [i for i in range(1, amount) if counts[i] < limit]
        pool, budget = sum([portions[i] for i in movable]), surplus
        for i in movable:
            addition = min(limit - counts[i], max(1, budget * portions[i] // pool), surplus)
            counts[i] = counts[i] + addition
            surplus = surplus - addition
    return np.array(counts)


def gaussian(own_key, dims, scale, limit, shards=(), held_as=jnp.bfloat16):
    entries = jax.random.normal(own_key, dims, jnp.float32) * scale
    if len(shards) > 0:
        entries = level_of(own_key, dims, shards, -0.22, 0.18) * entries
    return jnp.clip(entries, min=-limit, max=limit).astype(held_as)


def heavy_noise(key, shape, width, most, shards, heavy, kind=jnp.bfloat16):
    result = width * jax.random.normal(key, shape, jnp.float32)
    if shards:
        result = result * level_of(key, shape, shards, -0.22, 0.18)
    return jnp.clip(strengthened(result, jax.random.fold_in(key, 3), *heavy), -most, most).astype(kind)


def setup_inputs(seed: int = 0) -> dict:
    splits = jax.random.split(jax.random.key(seed), 17)
    q_latent = gaussian(splits[0], (TOKA * N_EP, QR), 1.0, 6.0, ((0, 8),))
    kv_latent = gaussian(splits[1], (TOKA * N_EP, KVR), 1.0, 6.0, ((0, 8),))
    rope_key = draw_rope_key(jax.random.fold_in(splits[16], 71), 0)
    q_gain = jnp.clip(1.0 + 0.18 * jax.random.normal(splits[3], (QR,), jnp.float32), 0.1, 1.9)
    kv_gain = jnp.clip(1.0 + 0.18 * jax.random.normal(splits[4], (KVR,), jnp.float32), 0.1, 1.9)
    w_query = gaussian(splits[5], (QR, HEADS * (NOPE + ROPE)), QR ** -0.5, 0.25, ((1, 4),))
    w_key = gaussian(splits[6], (KVR, HEADS * NOPE), KVR ** -0.5, 0.375, ((1, 4),))
    w_value = gaussian(splits[7], (KVR, HEADS * VDIM), KVR ** -0.5, 0.375, ((1, 4),))
    w_mix_out = gaussian(splits[8], (HEADS * VDIM, D), (HEADS * VDIM) ** -0.5, 0.125, ((0, 4),))
    expert_in = gaussian(splits[9], (TOKB * N_EP, D), 1.0, 6.0, ((0, 8),))
    norm_gain = jnp.clip(1.0 + 0.18 * jax.random.normal(splits[10], (D,), jnp.float32), 0.1, 1.9)
    routes_keys = jax.random.split(jax.random.fold_in(splits[11], 1), (TOKB * N_EP) // TOKB)
    routes_turns = jax.random.permutation(jax.random.fold_in(splits[11], 3), (TOKB * N_EP) // TOKB)
    routes = jax.vmap(lambda own, number: assign_block(jax.random.fold_in(splits[11], 2), own, number, TOKB, EXPERTS, TOP, CAP, 2))(routes_keys, routes_turns).reshape((TOKB * N_EP, TOP))
    route_scores = jnp.clip(jnp.exp(math.log(1.0) - 2.9957323 * jax.random.uniform(splits[12], (TOKB * N_EP, TOP), jnp.float32) ** level_of(splits[12], (TOKB * N_EP, TOP), ((0, 8),), -0.2, 0.2)), 0.05, 1.0)
    w_gate = gaussian(splits[13], (EXPERTS, D, FF), D ** -0.5, 0.125, ((0, 8), (2, 4)))
    w_up = gaussian(splits[14], (EXPERTS, D, FF), D ** -0.5, 0.125, ((0, 8), (2, 4)))
    w_down = heavy_noise(splits[15], (EXPERTS, FF, D), FF ** -0.5, 0.125, ((0, 8), (1, 4)), (1, 2, 4, 2.0))
    return {"q_latent": q_latent, "kv_latent": kv_latent, "rope_key": rope_key, "q_gain": q_gain, "kv_gain": kv_gain, "w_query": w_query, "w_key": w_key, "w_value": w_value, "w_mix_out": w_mix_out, "expert_in": expert_in, "norm_gain": norm_gain, "routes": routes, "route_scores": route_scores, "w_gate": w_gate, "w_up": w_up, "w_down": w_down}


eps_norm = 1e-05
rope_base = 10000.0

def rms_scale(values, gain):
    wide = values.astype(jnp.float32)
    return wide * lax.rsqrt(lax.optimization_barrier(jnp.mean(wide * wide, -1, keepdims=True)) + eps_norm) * gain

def rotate(values, cosine, sine):
    first, second = jnp.split(values, 2, axis=-1)
    return jnp.concatenate([first * cosine - second * sine, first * sine + second * cosine], -1)

def angles(positions):
    inverse = rope_base ** (-jnp.arange(0, ROPE, 2).astype(jnp.float32) / ROPE)
    phase = positions[:, None] * inverse[None, :]
    return (jnp.cos(phase), jnp.sin(phase))

def grouped_sum(left, right, groups):
    length = left.shape[0]
    inner = left.shape[1] // groups
    left_groups = jnp.transpose(left.reshape(length, groups, inner), (1, 0, 2))
    right_groups = right.reshape(groups, inner, right.shape[1])

    def add_group(total, pair):
        part = jnp.dot(pair[0], pair[1], preferred_element_type=jnp.float32).astype(jnp.bfloat16)
        part = lax.optimization_barrier(part)
        return (total + part.astype(jnp.float32), None)
    start_total = jnp.zeros((length, right.shape[1]), jnp.float32)
    total, unused = lax.scan(add_group, start_total, (left_groups, right_groups))
    return total.astype(jnp.bfloat16)

def reference(q_latent, kv_latent, rope_key, q_gain, kv_gain, w_query, w_key, w_value, w_mix_out, expert_in, norm_gain, routes, route_scores, w_gate, w_up, w_down):
    length = q_latent.shape[0]
    positions = jnp.arange(length, dtype=jnp.int32).astype(jnp.float32)
    cosine, sine = angles(positions)
    q_normed = rms_scale(q_latent, q_gain).astype(jnp.bfloat16)
    kv_normed = rms_scale(kv_latent, kv_gain).astype(jnp.bfloat16)
    query = jnp.dot(q_normed, w_query, preferred_element_type=jnp.float32).astype(jnp.bfloat16)
    query = query.reshape(length, HEADS, NOPE + ROPE)
    q_pass = query[:, :, :NOPE]
    q_rot = rotate(query[:, :, NOPE:].astype(jnp.float32), cosine[:, None, :], sine[:, None, :]).astype(jnp.bfloat16)
    k_rot = rotate(rope_key.astype(jnp.float32), cosine, sine).astype(jnp.bfloat16)
    keys = jnp.dot(kv_normed, w_key, preferred_element_type=jnp.float32).astype(jnp.bfloat16).reshape(length, HEADS, NOPE)
    values = jnp.dot(kv_normed, w_value, preferred_element_type=jnp.float32).astype(jnp.bfloat16).reshape(length, HEADS, VDIM)
    factor = (NOPE + ROPE) ** (-0.5)

    def attend_head(inputs):
        pass_head, rot_head, key_head, value_head = inputs
        scores = jnp.dot(pass_head, key_head.T, preferred_element_type=jnp.float32)
        scores = (scores + jnp.dot(rot_head, k_rot.T, preferred_element_type=jnp.float32)) * factor
        peak = lax.optimization_barrier(jnp.max(scores, -1, keepdims=True))
        weights = jnp.exp(scores - peak)
        total = lax.optimization_barrier(jnp.sum(weights, -1, keepdims=True))
        summed = jnp.dot(weights.astype(jnp.bfloat16), value_head, preferred_element_type=jnp.float32)
        return (summed / total).astype(jnp.bfloat16)
    per_head = lax.map(attend_head, (jnp.transpose(q_pass, (1, 0, 2)), jnp.transpose(q_rot, (1, 0, 2)), jnp.transpose(keys, (1, 0, 2)), jnp.transpose(values, (1, 0, 2))))
    attended = jnp.transpose(per_head, (1, 0, 2)).reshape(length, HEADS * VDIM)
    mixed = grouped_sum(attended, w_mix_out, N_TP)
    token_total = expert_in.shape[0]
    wide = expert_in.astype(jnp.float32)
    centered = wide - lax.optimization_barrier(jnp.mean(wide, -1, keepdims=True))
    normed = (centered * lax.rsqrt(lax.optimization_barrier(jnp.mean(centered * centered, -1, keepdims=True)) + eps_norm) * norm_gain).astype(jnp.bfloat16)
    shares = route_scores / lax.optimization_barrier(jnp.sum(route_scores, -1, keepdims=True))
    flat_expert = routes.reshape(-1).astype(jnp.int32)
    copies = flat_expert.shape[0]
    group_of = (jnp.arange(copies, dtype=jnp.int32) // (TOKB * TOP)).astype(jnp.int32)
    onehot = (flat_expert[:, None] == jnp.arange(EXPERTS, dtype=jnp.int32)[None, :]).astype(jnp.int32)
    within = onehot.reshape(N_EP, TOKB * TOP, EXPERTS)
    before = (jnp.cumsum(within, 1) - within).reshape(copies, EXPERTS)
    rank = lax.optimization_barrier(jnp.sum(before * onehot, 1)).astype(jnp.int32)
    slot = (group_of * CAP + rank).astype(jnp.int32)
    source = (jnp.arange(copies, dtype=jnp.int32) // TOP).astype(jnp.int32)
    table = jnp.full((EXPERTS, N_EP * CAP), token_total, jnp.int32).at[flat_expert, slot].set(source)
    padded = jnp.concatenate([normed, jnp.zeros((1, D), jnp.bfloat16)], 0)

    def one_expert(inputs):
        index, gate_weight, up_weight, down_weight = inputs
        arrived = padded[index]
        gate = jnp.dot(arrived, gate_weight, preferred_element_type=jnp.float32)
        up = jnp.dot(arrived, up_weight, preferred_element_type=jnp.float32)
        hidden = (jax.nn.silu(gate) * up).astype(jnp.bfloat16)
        return grouped_sum(hidden, down_weight, N_TP)
    results = lax.map(one_expert, (table, w_gate, w_up, w_down))
    picked = results[flat_expert, slot].astype(jnp.float32).reshape(token_total, TOP, D)
    expert_out = lax.optimization_barrier(jnp.sum(picked * shares[:, :, None], 1)).astype(jnp.bfloat16)
    return (mixed, expert_out)
```

```python
import functools

import jax
import jax.numpy as jnp
from jax import lax
from jax.experimental import pallas as pl
from jax.experimental.pallas import tpu as pltpu
from jax.sharding import PartitionSpec as P

NOPE = 128
ROPE = 64
VDIM = 128


eps_norm = 1e-05
rope_base = 10000.0


MESH = pl.DeviceIdType.MESH


def remote(src, dst, send, recv, ep, tp):
    return pltpu.make_async_remote_copy(
        src_ref=src, dst_ref=dst, send_sem=send, recv_sem=recv, device_id=(ep, tp), device_id_type=MESH
    )


def greet(ep_size, tp_size, me, part):
    barrier = pltpu.get_barrier_semaphore()
    for d in range(1, ep_size):
        pl.semaphore_signal(
            barrier, inc=1, device_id=(lax.rem(me + d, ep_size), part), device_id_type=MESH
        )
    for k in range(1, tp_size):
        pl.semaphore_signal(
            barrier, inc=1, device_id=(me, lax.rem(part + k, tp_size)), device_id_type=MESH
        )
    pl.semaphore_wait(barrier, ep_size + tp_size - 2)


def gather_kernel(
    ep_size, tp_size, kv, tok, tab, okv, otok, otab,
    z_send, z_recv, t_send, t_recv, c_send, c_recv, o_send, o_recv, b_send, b_recv, local,
):
    me = lax.axis_index("ep")
    part = lax.axis_index("tp")
    levels = ep_size // 2
    level, core = me // 2, me % 2
    twin = level * 2 + 1 - core
    greet(ep_size, tp_size, me, part)
    pairs = ((kv, okv), (tok, otok))
    waits = []
    own = [pltpu.make_async_copy(tab.at[me], otab.at[me], local.at[2])]
    for a, (src, dst) in enumerate(pairs):
        own.append(pltpu.make_async_copy(src, dst.at[me], local.at[a]))
    for copy in own:
        copy.start()
    order = [d for d in range(1, levels)]
    for a, (src, dst) in enumerate(pairs):
        for d in order:
            target = lax.rem(level + d, levels) * 2 + core
            copy = remote(
                src.at[part], dst.at[me, part], z_send.at[a, d], z_recv.at[a, d], target, part
            )
            copy.start()
            waits.append(copy)
        if a == 0:
            for d in range(1, ep_size):
                target = lax.rem(me + d, ep_size)
                copy = remote(
                    tab.at[target], otab.at[me], b_send.at[d], b_recv.at[d], target, part
                )
                copy.start()
                waits.append(copy)
    for a, (src, dst) in enumerate(pairs):
        copy = remote(src, dst.at[me], o_send.at[a], o_recv.at[a], twin, part)
        copy.start()
        waits.append(copy)
    for a, (src, dst) in enumerate(pairs):
        for d in order:
            block = lax.rem(level - d + levels, levels) * 2 + core
            here = dst.at[block, part]
            remote(here, here, z_send.at[a, d], z_recv.at[a, d], twin, part).wait_recv()
            for k in range(1, tp_size):
                copy = remote(
                    here, here, t_send.at[a, d, k], t_recv.at[a, d, k],
                    me, lax.rem(part + k, tp_size),
                )
                copy.start()
                waits.append(copy)
            copy = remote(here, here, c_send.at[a, d, 0], c_recv.at[a, d, 0], twin, part)
            copy.start()
            waits.append(copy)
    for a, (src, dst) in enumerate(pairs):
        for d in order:
            block = lax.rem(level - d + levels, levels) * 2 + core
            for k in range(1, tp_size):
                here = dst.at[block, lax.rem(part - k + tp_size, tp_size)]
                remote(here, here, t_send.at[a, d, k], t_recv.at[a, d, k], twin, part).wait_recv()
                copy = remote(here, here, c_send.at[a, d, k], c_recv.at[a, d, k], twin, part)
                copy.start()
                waits.append(copy)
    for a, (src, dst) in enumerate(pairs):
        remote(src, dst.at[twin], o_send.at[a], o_recv.at[a], twin, part).wait_recv()
        for d in order:
            block = lax.rem(level - d + levels, levels) * 2 + 1 - core
            for k in range(tp_size):
                here = dst.at[block, lax.rem(part - k + tp_size, tp_size)]
                remote(here, here, c_send.at[a, d, k], c_recv.at[a, d, k], twin, part).wait_recv()
    for d in range(1, ep_size):
        source = lax.rem(me - d + ep_size, ep_size)
        here = otab.at[source]
        remote(here, here, b_send.at[d], b_recv.at[d], twin, part).wait_recv()
    for copy in waits:
        copy.wait_send()
    for copy in own:
        copy.wait()


def vmem(count):
    return [pl.BlockSpec(memory_space=pltpu.VMEM)] * count


def gather_all(kv, tok, tab):
    ep_size, tp_size = lax.axis_size("ep"), lax.axis_size("tp")
    levels = ep_size // 2
    dma = pltpu.SemaphoreType.DMA
    return pl.pallas_call(
        functools.partial(gather_kernel, ep_size, tp_size),
        out_shape=(
            jax.ShapeDtypeStruct((ep_size,) + kv.shape, kv.dtype),
            jax.ShapeDtypeStruct((ep_size,) + tok.shape, tok.dtype),
            jax.ShapeDtypeStruct(tab.shape, tab.dtype),
        ),
        in_specs=vmem(3),
        out_specs=tuple(vmem(3)),
        scratch_shapes=[
            dma((2, levels)), dma((2, levels)),
            dma((2, levels, tp_size)), dma((2, levels, tp_size)),
            dma((2, levels, tp_size)), dma((2, levels, tp_size)),
            dma((2,)), dma((2,)), dma((ep_size,)), dma((ep_size,)), dma((3,)),
        ],
        compiler_params=pltpu.CompilerParams(
            collective_id=0, has_side_effects=True, vmem_limit_bytes=60 * 1024 * 1024
        ),
    )(kv, tok, tab)


def reduce_kernel(
    ep_size, tp_size, part_ref, mix, comb, mixed, landed, mix_landed, reduced,
    p_send, p_recv, m_send, m_recv, r_send, r_recv, local,
):
    me = lax.axis_index("ep")
    part = lax.axis_index("tp")
    greet(ep_size, tp_size, me, part)
    features = comb.shape[2]
    waits = []

    def columns(index):
        return pl.ds(pl.multiple_of(index * features, features), features)

    order = [(j + ep_size // 2) % ep_size for j in range(ep_size)]
    order = [j for j in order if j != 0] + [0]
    for j in order:
        block = lax.rem(me + j, ep_size)
        for k in range(1, tp_size):
            target = lax.rem(part + k, tp_size)
            copy = remote(
                part_ref.at[block, :, columns(target)], landed.at[k, block],
                p_send.at[j, k], p_recv.at[j, k], me, target,
            )
            copy.start()
            waits.append(copy)
    for k in range(1, tp_size):
        target = lax.rem(part + k, tp_size)
        copy = remote(mix.at[target], mix_landed.at[k], m_send.at[k], m_recv.at[k], me, target)
        copy.start()
        waits.append(copy)
    for j in order:
        block = lax.rem(me + j, ep_size)
        total = part_ref[block, :, columns(part)].astype(jnp.float32)
        for k in range(1, tp_size):
            here = landed.at[k, block]
            remote(here, here, p_send.at[j, k], p_recv.at[j, k], me, part).wait_recv()
            total = total + landed[k, block].astype(jnp.float32)
        if j == 0:
            comb[me] = total.astype(jnp.bfloat16)
        else:
            reduced[block] = total.astype(jnp.bfloat16)
            copy = remote(
                reduced.at[block], comb.at[me], r_send.at[j], r_recv.at[j], block, part
            )
            copy.start()
            waits.append(copy)
    total = mix[part].astype(jnp.float32)
    for k in range(1, tp_size):
        here = mix_landed.at[k]
        remote(here, here, m_send.at[k], m_recv.at[k], me, part).wait_recv()
        total = total + mix_landed[k].astype(jnp.float32)
    mixed[...] = total.astype(jnp.bfloat16)
    for j in range(1, ep_size):
        here = comb.at[lax.rem(me - j + ep_size, ep_size)]
        remote(here, here, r_send.at[j], r_recv.at[j], me, part).wait_recv()
    for copy in waits:
        copy.wait_send()


def reduce_all(part, mix):
    ep_size, tp_size = lax.axis_size("ep"), lax.axis_size("tp")
    slots, width = part.shape[1:]
    features = width // tp_size
    dma = pltpu.SemaphoreType.DMA
    return pl.pallas_call(
        functools.partial(reduce_kernel, ep_size, tp_size),
        out_shape=(
            jax.ShapeDtypeStruct((ep_size, slots, features), jnp.bfloat16),
            jax.ShapeDtypeStruct(mix.shape[1:], jnp.bfloat16),
        ),
        in_specs=vmem(2),
        out_specs=tuple(vmem(2)),
        scratch_shapes=[
            pltpu.VMEM((tp_size, ep_size, slots, features), jnp.bfloat16),
            pltpu.VMEM(mix.shape, jnp.bfloat16),
            pltpu.VMEM((ep_size, slots, features), jnp.bfloat16),
            dma((ep_size, tp_size)), dma((ep_size, tp_size)),
            dma((tp_size,)), dma((tp_size,)), dma((ep_size,)), dma((ep_size,)), dma((1,)),
        ],
        compiler_params=pltpu.CompilerParams(
            collective_id=1, has_side_effects=True, vmem_limit_bytes=60 * 1024 * 1024
        ),
    )(part, mix)


def rms_scale(values, gain):
    wide = values.astype(jnp.float32)
    return wide * lax.rsqrt(jnp.mean(wide * wide, -1, keepdims=True) + eps_norm) * gain


def rotate(values, cosine, sine):
    first, second = jnp.split(values, 2, axis=-1)
    return jnp.concatenate([first * cosine - second * sine, first * sine + second * cosine], -1)


def angles(positions):
    inverse = rope_base ** (-jnp.arange(0, ROPE, 2).astype(jnp.float32) / ROPE)
    phase = positions[:, None] * inverse[None, :]
    return (jnp.cos(phase), jnp.sin(phase))


def latents(kv_latent, rope_key, kv_gain):
    token_count = kv_latent.shape[0]
    offset = lax.axis_index("ep") * token_count
    positions = (offset + jnp.arange(token_count, dtype=jnp.int32)).astype(jnp.float32)
    cosine, sine = angles(positions)
    kv_normed = rms_scale(kv_latent, kv_gain).astype(jnp.bfloat16)
    key_turned = rotate(rope_key.astype(jnp.float32), cosine, sine).astype(jnp.bfloat16)
    width = kv_latent.shape[1] + rope_key.shape[1]
    spare = jnp.zeros((token_count, -width % 128), jnp.bfloat16)
    return jnp.concatenate([kv_normed, key_turned, spare], 1), cosine, sine


def queries(q_latent, q_gain, w_query, cosine, sine):
    token_count = q_latent.shape[0]
    head_count = w_query.shape[1] // (NOPE + ROPE)
    q_normed = rms_scale(q_latent, q_gain).astype(jnp.bfloat16)
    query = jnp.dot(q_normed, w_query, preferred_element_type=jnp.float32).astype(jnp.bfloat16)
    query = query.reshape(token_count, head_count, NOPE + ROPE)
    q_pass = query[:, :, :NOPE]
    q_turned = rotate(
        query[:, :, NOPE:].astype(jnp.float32), cosine[:, None, :], sine[:, None, :]
    ).astype(jnp.bfloat16)
    return q_pass, q_turned


def attend(q_pass, q_turned, latent, turned, w_key, w_value, w_mix_out):
    token_count, head_count = q_pass.shape[:2]
    factor = (NOPE + ROPE) ** (-0.5)
    count = latent.shape[0]
    keys = jnp.dot(latent, w_key, preferred_element_type=jnp.float32).astype(jnp.bfloat16)
    keys = keys.reshape(count, head_count, NOPE)
    values = jnp.dot(latent, w_value, preferred_element_type=jnp.float32).astype(jnp.bfloat16)
    values = values.reshape(count, head_count, VDIM)
    scores = jnp.einsum("qhd,khd->hqk", q_pass, keys, preferred_element_type=jnp.float32)
    scores = (
        scores + jnp.einsum("qhd,kd->hqk", q_turned, turned, preferred_element_type=jnp.float32)
    ) * factor
    peak = jnp.max(scores, -1)
    weights = jnp.exp(scores - peak[:, :, None])
    total = jnp.sum(weights, -1)
    summed = jnp.einsum(
        "hqk,khd->qhd", weights.astype(jnp.bfloat16), values, preferred_element_type=jnp.float32
    )
    attended = (summed / jnp.transpose(total)[:, :, None]).astype(jnp.bfloat16)
    attended = attended.reshape(token_count, head_count * VDIM)
    return jnp.dot(attended, w_mix_out, preferred_element_type=jnp.float32).astype(jnp.bfloat16)


def routing(routes):
    token_count, choose = routes.shape
    expert_count = lax.axis_size("ep")
    slots = 2 * choose * token_count // expert_count
    flat_expert = routes.reshape(-1)
    onehot = (flat_expert[:, None] == jnp.arange(expert_count, dtype=jnp.int32)[None, :]).astype(
        jnp.int32
    )
    before = jnp.sum((jnp.cumsum(onehot, 0) - onehot) * onehot, 1)
    target = flat_expert * slots + before
    source = jnp.arange(token_count * choose, dtype=jnp.int32) // choose
    table = jnp.zeros((expert_count * slots,), jnp.int32).at[target].set(source)
    table = table.reshape(expert_count, 1, slots)
    table = jnp.pad(table, ((0, 0), (0, 7), (0, -slots % 128)))
    return target, table, slots


def normalize(expert_in, norm_gain):
    wide = expert_in.astype(jnp.float32)
    centered = wide - jnp.mean(wide, -1, keepdims=True)
    return (
        centered
        * lax.rsqrt(jnp.mean(centered * centered, -1, keepdims=True) + eps_norm)
        * norm_gain
    ).astype(jnp.bfloat16)


def body(
    q_latent,
    kv_latent,
    rope_key,
    q_gain,
    kv_gain,
    w_query,
    w_key,
    w_value,
    w_mix_out,
    expert_in,
    norm_gain,
    routes,
    route_scores,
    w_gate,
    w_up,
    w_down,
):
    ep_size, tp_size = lax.axis_size("ep"), lax.axis_size("tp")
    token_count, width = expert_in.shape
    choose = routes.shape[1]
    target, table, slots = routing(routes)
    normed = normalize(expert_in, norm_gain)
    packed, cosine, sine = latents(kv_latent, rope_key, kv_gain)
    all_packed, all_normed, arrived_table = gather_all(
        packed.reshape(tp_size, -1, packed.shape[1]), normed.reshape(tp_size, -1, width), table
    )
    rank = kv_latent.shape[1]
    all_packed = all_packed.reshape(-1, packed.shape[1])
    latent, turned = all_packed[:, :rank], all_packed[:, rank : rank + ROPE]
    q_pass, q_turned = queries(q_latent, q_gain, w_query, cosine, sine)
    mix = attend(q_pass, q_turned, latent, turned, w_key, w_value, w_mix_out)
    index = arrived_table[:, 0, :slots] + jnp.arange(ep_size, dtype=jnp.int32)[:, None] * token_count
    arrived = jnp.take(all_normed.reshape(-1, width), index.reshape(-1), axis=0, mode="clip")
    gate = jnp.dot(arrived, w_gate[0], preferred_element_type=jnp.float32)
    up = jnp.dot(arrived, w_up[0], preferred_element_type=jnp.float32)
    hidden = (jax.nn.silu(gate) * up).astype(jnp.bfloat16)
    part = jnp.dot(hidden, w_down[0], preferred_element_type=jnp.float32).astype(jnp.bfloat16)
    comb, mixed = reduce_all(
        part.reshape(ep_size, slots, width), mix.reshape(tp_size, -1, mix.shape[1])
    )
    shares = route_scores / jnp.sum(route_scores, -1, keepdims=True)
    picked = jnp.take(comb.reshape(ep_size * slots, -1), target, axis=0, mode="clip")
    picked = picked.reshape(token_count, choose, -1).astype(jnp.float32)
    expert_out = jnp.sum(picked * shares[:, :, None], 1).astype(jnp.bfloat16)
    return (mixed, expert_out)


def solution(mesh):
    in_specs = (
        P("ep", None),
        P("ep", None),
        P("ep", None),
        P(),
        P(),
        P(None, "tp"),
        P(None, "tp"),
        P(None, "tp"),
        P("tp", None),
        P("ep", None),
        P(),
        P("ep", None),
        P("ep", None),
        P("ep", None, "tp"),
        P("ep", None, "tp"),
        P("ep", "tp", None),
    )
    out_specs = (P(("ep", "tp"), None), P("ep", "tp"))
    return jax.shard_map(body, mesh=mesh, in_specs=in_specs, out_specs=out_specs, check_vma=False)
```
